32 devices in a mesh: sp: 8 (over z, y), tp: 4 (over x, core).
Axes of the slice: x: 2, y: 2, z: 4, core: 2. Of those that a mesh axis runs over, the one named last changes fastest.
Arguments:
- mixer_input: bfloat16 [2048, 1024], P('sp', 'tp'), may hold values from -6 to 6
- retention: float32 [64, 2048], P('tp', 'sp'), may hold values from -1 to 0
- decay_real: float32 [64, 64], P('tp'), may hold values from -0.7 to -0.3
- decay_freq: float32 [64, 64], P('tp'), may hold values from 0 to 26
- log_step: float32 [64], P('tp')
- input_real: float32 [64, 64, 16], P('tp')
- input_imag: float32 [64, 64, 16], P('tp')
- readout_real: float32 [64, 16, 64], P('tp'), may hold values from -0.5 to 0.5
- readout_imaginary: float32 [64, 16, 64], P('tp'), may hold values from -0.5 to 0.5
- skip_weight: float32 [64, 16], P('tp'), may hold values from -4 to 4
- norm_gain: float32 [1024], replicated, may hold values from 0.1 to 1.9
- projection: bfloat16 [1024, 2048], P('tp'), may hold values from -0.1875 to 0.1875
- residual: bfloat16 [2048, 2048], P(('sp', 'tp')), may hold values from -6 to 6
- mix_gain: float32 [2048], replicated, may hold values from 0.1 to 1.9
- routes: int32 [2048, 2], P(('sp', 'tp')), may hold values from 0 to 7, all different within a row; in each aligned block of 64 rows (0 to 63, 64 to 127, ...) at most 32 rows name the same one
- route_weight: float32 [2048, 2], P(('sp', 'tp')), may hold values from 0.5 to 2
- expert_gate: bfloat16 [8, 2048, 512], P('sp'), may hold values from -0.125 to 0.125
- expert_up: bfloat16 [8, 2048, 512], P('sp'), may hold values from -0.125 to 0.125
- expert_down: bfloat16 [8, 512, 2048], P('sp'), may hold values from -0.25 to 0.25
- final_gain: float32 [2048], replicated, may hold values from 0.1 to 1.9
Outputs:
- layer_out: bfloat16 [2048, 2048], P(('sp', 'tp'))
The draws below stay inside these ranges and needn't reach their ends.
Inputs may be any that keep to these rules, and one draw needn't show every extreme that they name: `routes`: in each aligned block of 64 rows no expert is named by more than 32 rows, and in some blocks one is named by exactly 32 rows; each row names 2 different experts.
All inputs are finite; a program needn't handle non-finite values.
Results may differ from the reference program's by a relative error of at most 0.017.
Values may be sent and summed in bfloat16 or wider, within the bound.
No kernel may reach another device: no remote copies, remote signals or barrier semaphores. Data moves between devices by JAX's collectives and lax.ppermute only.
A program may use at most 64 MiB of HBM per device.

```python
import math
import jax
import jax.numpy as jnp
import numpy as np
from jax import lax

WIDTH = 2048
GROUPS = 64
CHANNELS = 16
STATE = 64
EXPERT_HIDDEN = 512
PICKS = 2
SHARD_TOKENS = 256
MIX_WIDTH = 1024
SEQUENCE_TOKENS = 2048
DEVICE_ROWS = 64
EXPERTS = 8
CAPACITY = 32


def decay_plan(key):
    folded_values = jax.random.fold_in(key, 7)
    slow_share = 0.5
    slow_group = jax.random.uniform(jax.random.fold_in(folded_values, 1), (GROUPS,), jnp.float32) < slow_share
    decay_real = -jax.random.uniform(jax.random.fold_in(folded_values, 2), (GROUPS, STATE), jnp.float32, 0.3, 0.7)
    decay_freq = jax.random.uniform(jax.random.fold_in(folded_values, 3), (GROUPS, STATE), jnp.float32, 0.0, 8.0 * math.pi)
    fast_log = jax.random.uniform(jax.random.fold_in(folded_values, 4), (GROUPS,), jnp.float32, math.log(0.04), math.log(0.12))
    slow_log = jax.random.uniform(jax.random.fold_in(folded_values, 5), (GROUPS,), jnp.float32, math.log(0.2 / SEQUENCE_TOKENS), math.log(0.6 / SEQUENCE_TOKENS))
    log_step = jnp.where(slow_group, slow_log, fast_log)
    stride = jnp.exp(log_step)[:, None]
    growth = decay_real * stride
    turning = decay_freq * stride
    upper_real = jnp.expm1(growth) * jnp.cos(turning) - 2.0 * jnp.sin(0.5 * turning) ** 2
    upper_imag = jnp.exp(growth) * jnp.sin(turning)
    magnitude = jnp.sqrt(upper_real * upper_real + upper_imag * upper_imag)
    magnitude = magnitude / jnp.sqrt(decay_real * decay_real + decay_freq * decay_freq)
    scaling = jnp.sqrt(-2.0 * growth) / magnitude / math.sqrt(CHANNELS)
    return (decay_real, decay_freq, log_step, scaling)


def draw_decay_real(key, part):
    return decay_plan(key)[0]


def draw_decay_freq(key, part):
    return decay_plan(key)[1]


def draw_log_step(key, part):
    return decay_plan(key)[2]


def draw_input_real(key, part):
    scaling = decay_plan(key)[3]
    return scaling[:, :, None] * jax.random.normal(jax.random.fold_in(key, 21), (GROUPS, STATE, CHANNELS), jnp.float32)


def draw_input_imag(key, part):
    scaling = decay_plan(key)[3]
    return scaling[:, :, None] * jax.random.normal(jax.random.fold_in(key, 22), (GROUPS, STATE, CHANNELS), jnp.float32)


def draw_retention(key, part):
    folded_values = jax.random.fold_in(key, 13)
    blocks = SEQUENCE_TOKENS // SHARD_TOKENS
    factor = jnp.exp(jax.random.uniform(jax.random.fold_in(folded_values, 1), (GROUPS, blocks), jnp.float32, 0.0, math.log(4.0)))
    roughness = jax.random.uniform(jax.random.fold_in(folded_values, 2), (GROUPS, SEQUENCE_TOKENS), jnp.float32, 0.5, 1.5)
    base_level = 0.2
    steady_state = -(base_level / SEQUENCE_TOKENS) * jnp.repeat(factor, SHARD_TOKENS, axis=1) * roughness
    spike_locations = jax.random.randint(jax.random.fold_in(folded_values, 3), (3,), 0, SEQUENCE_TOKENS)
    loss_values = jnp.log(jax.random.uniform(jax.random.fold_in(folded_values, 4), (3, GROUPS), jnp.float32, 0.65, 0.8))
    spike_mask = (jnp.arange(SEQUENCE_TOKENS)[None, :] == spike_locations[:, None]).astype(jnp.float32)
    return steady_state + jnp.einsum('aw,ay->wy', loss_values, spike_mask)


def steps_of(rng, dims, pieces, low, largest):
    loudness, own = 1.0, jax.random.fold_in(rng, 6)
    for dim, parts in pieces:
        heights = jnp.exp(jax.random.uniform(jax.random.fold_in(own, dim), (parts,), jnp.float32, low / len(pieces), largest / len(pieces)))
        loudness = loudness * jnp.repeat(heights, dims[dim] // parts).reshape([-1 if axis == dim else 1 for axis in range(len(dims))])
    return loudness


def shared_out(rng, own, number, rows, amount, top, most, skew):
    sequence = jax.random.permutation(rng, amount)
    heavy_load, usual = portions_of(amount, rows * top, most, skew, True), portions_of(amount, rows * top, most, skew, False)
    places = jnp.arange(amount)

    def named(tallies, turn):
        used = int((tallies > 0).sum())
        fixed = max(1, used // 4)
        moved = fixed + (places - fixed + turn * (used - fixed)) % max(1, amount - fixed)
        return jnp.zeros((amount,), jnp.int32).at[sequence[jnp.where(places < fixed, places, moved)]].set(jnp.asarray(tallies, jnp.int32))

    tallies = jnp.where(number % 4 == 0, named(heavy_load, number // 4), named(usual, number - number // 4 - 1))
    mixed = jax.random.permutation(jax.random.fold_in(own, 3), amount)
    source_of, receiver = mixed[0:amount // 2 * 2:2], mixed[1:amount // 2 * 2:2]
    margin = jnp.minimum(tallies[source_of] - 1, most - tallies[receiver]) // 2
    margin = jnp.where((source_of == sequence[0]) | (receiver == sequence[0]) | (tallies[receiver] == 0), 0, jnp.maximum(margin, 0))
    moved = jax.random.randint(jax.random.fold_in(own, 4), (amount // 2,), 0, 1 << 20) % (margin + 1)
    tallies = tallies.at[source_of].add(-moved).at[receiver].add(moved)
    labels = jnp.searchsorted(jnp.cumsum(tallies), jnp.arange(rows * top), side="right").astype(jnp.int32)
    listing = labels.reshape(top, rows).T
    listing = listing[jax.random.permutation(jax.random.fold_in(own, 1), rows)]
    turn = jax.random.randint(jax.random.fold_in(own, 2), (rows, 1), 0, top)
    return jnp.take_along_axis(listing, (jnp.arange(top)[None, :] + turn) % top, axis=1)


def portions_of(amount, total, most, slope, full):
    loads = [(1 << 20) // math.isqrt(rank ** slope) + 1 for rank in range(1, amount + 1)]
    largest = most if full else min(most, max(-(-total // amount), total * loads[0] // sum(loads)))
    least = 1 if total - largest >= amount - 1 else 0
    given, surplus = [largest] + [least] * (amount - 1), total - largest - least * (amount - 1)
    while surplus > 0:
        candidates = [i for i in range(1, amount) if given[i] < largest] or [i for i in range(1, amount) if given[i] < most]
        mass, budget = sum([loads[i] for i in candidates]), surplus
        for i in candidates:
            more = min(most - given[i], max(1, budget * loads[i] // mass), surplus)
            given[i] = given[i] + more
            surplus = surplus - more
    return np.array(given)


def noise(own_key, shape, width, reach, split=(), kind=jnp.bfloat16):
    gain = steps_of(own_key, shape, split, -0.22, 0.18) if split else 1.0
    drawn = jax.random.normal(own_key, shape, jnp.float32) * width * gain
    return jnp.minimum(jnp.maximum(drawn, -reach), reach).astype(kind)


def setup_inputs(seed: int = 0) -> dict:
    seeds = jax.random.split(jax.random.key(seed), 21)
    mixer_input = noise(seeds[0], (SEQUENCE_TOKENS, MIX_WIDTH), 1.0, 6.0, ((0, 8), (1, 4)))
    retention = draw_retention(jax.random.fold_in(seeds[20], 71), 0)
    decay_real = draw_decay_real(jax.random.fold_in(seeds[20], 71), 0)
    decay_freq = draw_decay_freq(jax.random.fold_in(seeds[20], 71), 0)
    log_step = draw_log_step(jax.random.fold_in(seeds[20], 71), 0)
    input_real = draw_input_real(jax.random.fold_in(seeds[20], 71), 0)
    input_imag = draw_input_imag(jax.random.fold_in(seeds[20], 71), 0)
    readout_real = noise(seeds[7], (GROUPS, CHANNELS, STATE), (2 * STATE) ** -0.5, 0.5, ((0, 4),), jnp.float32)
    readout_imaginary = noise(seeds[8], (GROUPS, CHANNELS, STATE), (2 * STATE) ** -0.5, 0.5, ((0, 4),), jnp.float32)
    skip_weight = noise(seeds[9], (GROUPS, CHANNELS), 1.0, 4.0, ((0, 4),), jnp.float32)
    norm_gain = jnp.clip(1.0 + 0.18 * jax.random.normal(seeds[10], (MIX_WIDTH,), jnp.float32), 0.1, 1.9)
    projection = noise(seeds[11], (MIX_WIDTH, WIDTH), MIX_WIDTH ** -0.5, 0.1875, ((0, 4),))
    residual = noise(seeds[12], (SEQUENCE_TOKENS, WIDTH), 1.0, 6.0, ((0, 32),))
    mix_gain = jnp.clip(1.0 + 0.18 * jax.random.normal(seeds[13], (WIDTH,), jnp.float32), 0.1, 1.9)
    routes_keys = jax.random.split(jax.random.fold_in(seeds[14], 1), SEQUENCE_TOKENS // DEVICE_ROWS)
    routes_turns = jax.random.permutation(jax.random.fold_in(seeds[14], 3), SEQUENCE_TOKENS // DEVICE_ROWS)
    routes = jax.vmap(lambda own, number: shared_out(jax.random.fold_in(seeds[14], 2), own, number, DEVICE_ROWS, EXPERTS, PICKS, CAPACITY, 2))(routes_keys, routes_turns).reshape((SEQUENCE_TOKENS, PICKS))
    route_weight = jnp.clip(0.5 + 1.5 * jax.random.uniform(seeds[15], (SEQUENCE_TOKENS, PICKS), jnp.float32) ** steps_of(seeds[15], (SEQUENCE_TOKENS, PICKS), ((0, 32),), -0.2, 0.2), 0.5, 2.0)
    expert_gate = noise(seeds[16], (EXPERTS, WIDTH, EXPERT_HIDDEN), WIDTH ** -0.5, 0.125, ((0, 8),))
    expert_up = noise(seeds[17], (EXPERTS, WIDTH, EXPERT_HIDDEN), WIDTH ** -0.5, 0.125, ((0, 8),))
    expert_down = noise(seeds[18], (EXPERTS, EXPERT_HIDDEN, WIDTH), EXPERT_HIDDEN ** -0.5, 0.25, ((0, 8),))
    final_gain = jnp.clip(1.0 + 0.18 * jax.random.normal(seeds[19], (WIDTH,), jnp.float32), 0.1, 1.9)
    return dict(mixer_input=mixer_input, retention=retention, decay_real=decay_real, decay_freq=decay_freq, log_step=log_step, input_real=input_real, input_imag=input_imag, readout_real=readout_real, readout_imaginary=readout_imaginary, skip_weight=skip_weight, norm_gain=norm_gain, projection=projection, residual=residual, mix_gain=mix_gain, routes=routes, route_weight=route_weight, expert_gate=expert_gate, expert_up=expert_up, expert_down=expert_down, final_gain=final_gain)


deep_alpha = 2.0 ** 0.25
highest_precision = lax.Precision.HIGHEST
row_block = 512

def input_factor(decay_real, decay_freq, log_step):
    stride = jnp.exp(log_step)[:, None]
    growth = decay_real * stride
    turning = decay_freq * stride
    upper_real = jnp.expm1(growth) * jnp.cos(turning) - 2.0 * jnp.sin(0.5 * turning) ** 2
    upper_imag = jnp.exp(growth) * jnp.sin(turning)
    denominator = decay_real * decay_real + decay_freq * decay_freq
    factor_real = (upper_real * decay_real + upper_imag * decay_freq) / denominator
    factor_imag = (upper_imag * decay_real - upper_real * decay_freq) / denominator
    return (growth, turning, factor_real, factor_imag)

def layer_norm(values, scales):
    centered = values - lax.optimization_barrier(jnp.mean(values, axis=-1, keepdims=True))
    variance = lax.optimization_barrier(jnp.mean(centered * centered, axis=-1, keepdims=True))
    return centered * lax.rsqrt(variance + 1e-05) * scales

def reference(mixer_input, retention, decay_real, decay_freq, log_step, input_real, input_imag, readout_real, readout_imaginary, skip_weight, norm_gain, projection, residual, mix_gain, routes, route_weight, expert_gate, expert_up, expert_down, final_gain):
    growth, turning, factor_real, factor_imag = input_factor(decay_real, decay_freq, log_step)
    keep_real = jnp.exp(growth) * jnp.cos(turning)
    keep_imag = jnp.exp(growth) * jnp.sin(turning)
    bar_real = factor_real[:, :, None] * input_real - factor_imag[:, :, None] * input_imag
    bar_imag = factor_real[:, :, None] * input_imag + factor_imag[:, :, None] * input_real
    inputs = mixer_input.reshape(SEQUENCE_TOKENS, GROUPS, CHANNELS)
    held_log = jnp.transpose(retention)

    def advance(carried, position):
        state_real_part, state_imaginary = carried
        current, kept_log = position
        current = current.astype(jnp.float32)
        shrink = jnp.exp(kept_log)[:, None]
        drive_real = jnp.einsum('gpc,gc->gp', bar_real, current, precision=highest_precision)
        drive_imag = jnp.einsum('gpc,gc->gp', bar_imag, current, precision=highest_precision)
        following_real = shrink * (keep_real * state_real_part - keep_imag * state_imaginary) + drive_real
        following_imaginary = shrink * (keep_real * state_imaginary + keep_imag * state_real_part) + drive_imag
        readout_result = jnp.einsum('zhy,zy->zh', readout_real, following_real, precision=highest_precision)
        readout_result = readout_result - jnp.einsum('zhy,zy->zh', readout_imaginary, following_imaginary, precision=highest_precision)
        readout_result = readout_result + skip_weight * current
        return ((following_real, following_imaginary), jax.nn.gelu(readout_result).astype(jnp.bfloat16))
    zero_state = jnp.zeros((GROUPS, STATE), jnp.float32)
    ignored_state, mixed_seq = lax.scan(advance, (zero_state, zero_state), (inputs, held_log))
    mixed_seq = mixed_seq.reshape(SEQUENCE_TOKENS, MIX_WIDTH)
    mixed_float = mixed_seq.astype(jnp.float32)
    row_square = lax.optimization_barrier(jnp.mean(mixed_float * mixed_float, axis=1))
    scaled = (mixed_float * norm_gain).astype(jnp.bfloat16)
    mix = jnp.dot(scaled, projection, preferred_element_type=jnp.float32) * lax.rsqrt(row_square + 1e-06)[:, None]
    hidden = layer_norm(deep_alpha * residual.astype(jnp.float32) + mix, mix_gain).astype(jnp.bfloat16)
    hidden_pad = jnp.concatenate([hidden, jnp.zeros((1, WIDTH), hidden.dtype)], axis=0)
    assigned = routes.reshape(-1).astype(jnp.int32)
    sort_order = jnp.argsort(assigned, stable=True).astype(jnp.int32)
    sorted_expert = assigned[sort_order]
    sorted_token = (sort_order // PICKS).astype(jnp.int32)
    sorted_weight = route_weight.reshape(-1)[sort_order]
    expert_load = lax.optimization_barrier(jnp.sum((assigned[:, None] == jnp.arange(EXPERTS, dtype=jnp.int32)[None, :]).astype(jnp.int32), axis=0))
    padded_rows = (expert_load + row_block - 1) // row_block * row_block
    padded_end = jnp.cumsum(padded_rows).astype(jnp.int32)
    padded_start = padded_end - padded_rows
    first_sorted = (jnp.cumsum(expert_load) - expert_load).astype(jnp.int32)
    assigned_count = SEQUENCE_TOKENS * PICKS
    dest_slot = padded_start[sorted_expert] + jnp.arange(assigned_count, dtype=jnp.int32) - first_sorted[sorted_expert]
    block_total = (assigned_count + EXPERTS * row_block) // row_block + 1
    buffer_rows = block_total * row_block
    token_buffer = jnp.full((buffer_rows,), SEQUENCE_TOKENS, jnp.int32).at[dest_slot].set(sorted_token)
    weight_buffer = jnp.zeros((buffer_rows,), route_weight.dtype).at[dest_slot].set(sorted_weight)
    block_starts = jnp.arange(block_total, dtype=jnp.int32) * row_block
    block_expert = lax.optimization_barrier(jnp.sum((padded_end[None, :] <= block_starts[:, None]).astype(jnp.int32), axis=1))
    block_expert = jnp.minimum(block_expert, EXPERTS - 1).astype(jnp.int32)

    def one_block(running, block_items):
        tokens_here, weights_here, expert_here = block_items
        rows_here = hidden_pad[tokens_here]
        gate_act = jnp.dot(rows_here, expert_gate[expert_here], preferred_element_type=jnp.float32)
        up_act = jnp.dot(rows_here, expert_up[expert_here], preferred_element_type=jnp.float32)
        active = (jax.nn.silu(gate_act) * up_act).astype(jnp.bfloat16)
        produced = jnp.dot(active, expert_down[expert_here], preferred_element_type=jnp.float32).astype(jnp.bfloat16)
        return (running.at[tokens_here].add(weights_here[:, None] * produced.astype(jnp.float32)), None)
    mix_init = jnp.zeros((SEQUENCE_TOKENS + 1, WIDTH), jnp.float32)
    expert_mix, ignored = lax.scan(one_block, mix_init, (token_buffer.reshape(block_total, row_block), weight_buffer.reshape(block_total, row_block), block_expert))
    layer_out = layer_norm(deep_alpha * hidden.astype(jnp.float32) + expert_mix[:SEQUENCE_TOKENS], final_gain)
    return layer_out.astype(jnp.bfloat16)
```

```python
import functools

import jax
import jax.numpy as jnp
from jax import lax
from jax.experimental import pallas as pl
from jax.experimental.pallas import tpu as pltpu
from jax.sharding import PartitionSpec as P

PICKS = 2
deep_alpha = 2.0**0.25
lanes_of_chunks = 8
f32, bf16 = jnp.float32, jnp.bfloat16
VMEM = pltpu.VMEM


def power_of_two(count):
    return count & (count - 1) == 0


def swap(value, axis, distance):
    count = lax.axis_size(axis)
    return lax.ppermute(value, axis, [(i, i ^ distance) for i in range(count)])


def shift(value, axis, distance):
    count = lax.axis_size(axis)
    return lax.ppermute(value, axis, [(i, (i + distance) % count) for i in range(count)])


def pieces(value, count):
    out = []
    for _ in range(count):
        piece = value.astype(bf16)
        out.append(piece)
        value = value - piece.astype(f32)
    return out


def nt(left, right):
    return lax.dot_general(left, right, (((1,), (1,)), ((), ())), preferred_element_type=f32)


def nn(left, right):
    return lax.dot_general(left, right, (((1,), (0,)), ((), ())), preferred_element_type=f32)


def tn(left, right):
    return lax.dot_general(left, right, (((0,), (0,)), ((), ())), preferred_element_type=f32)


def reorder(count):
    steps = count // lanes_of_chunks
    row = lax.broadcasted_iota(jnp.int32, (count, count), 0)
    col = lax.broadcasted_iota(jnp.int32, (count, count), 1)
    source = (row % lanes_of_chunks) * steps + row // lanes_of_chunks
    return jnp.where(col == source, 1.0, 0.0).astype(bf16)


def lane_row(value):
    groups, width = value.shape
    per = 128 // width
    wide = jnp.concatenate([value] * per, axis=1)
    spot = lax.broadcasted_iota(jnp.int32, (1, 128), 1) // width
    parts = []
    for q in range(groups // per):
        row = wide[q * per : q * per + 1]
        for m in range(1, per):
            row = jnp.where(spot == m, wide[q * per + m : q * per + m + 1], row)
        parts.append(row)
    return jnp.concatenate(parts, axis=1)


def complex_times(ar, ai, br, bi):
    return ar * br - ai * bi, ar * bi + ai * br


def less_one(value):
    near = jnp.ones_like(value)
    for k in range(11, 1, -1):
        near = 1.0 + near * value / k
    return jnp.where(jnp.abs(value) < 0.5, near * value, jnp.exp(value) - 1.0)


def advance(block_r, block_i, shrink, keep_r, keep_i, drive_r, drive_i):
    turned_r, turned_i = complex_times(keep_r, keep_i, block_r, block_i)
    return shrink * turned_r + drive_r, shrink * turned_i + drive_i


def drive_kernel(
    u_ref, held_ref, real_ref, freq_ref, step_ref, in_r_ref, in_i_ref,
    drive_ref, shrink_ref, chunk_ref, total_ref,
):
    tokens, _ = u_ref.shape
    groups, states = real_ref.shape
    channels = in_r_ref.shape[1]
    width = groups * states
    steps = tokens // lanes_of_chunks
    log_step = step_ref[...]
    eye = lax.broadcasted_iota(jnp.int32, (groups, groups), 0) == lax.broadcasted_iota(
        jnp.int32, (groups, groups), 1
    )
    log_column = jnp.sum(jnp.where(eye, log_step, 0.0), axis=1, keepdims=True)
    stride = jnp.exp(log_column)
    decay_real, decay_freq = real_ref[...], freq_ref[...]
    growth = decay_real * stride
    turning = decay_freq * stride
    size = jnp.exp(growth)
    cosine, sine, half = jnp.cos(turning), jnp.sin(turning), jnp.sin(0.5 * turning)
    upper_real = less_one(growth) * cosine - 2.0 * half * half
    upper_imag = size * sine
    denominator = decay_real * decay_real + decay_freq * decay_freq
    factor_real = (upper_real * decay_real + upper_imag * decay_freq) / denominator
    factor_imag = (upper_imag * decay_real - upper_real * decay_freq) / denominator
    keep_r, keep_i = lane_row(size * cosine), lane_row(upper_imag)
    factor_r, factor_i = lane_row(factor_real), lane_row(factor_imag)

    order = reorder(tokens)
    moved = nn(order, u_ref[...])
    held = jnp.concatenate(pieces(jnp.exp(held_ref[...]), 3), axis=0)
    held = nt(held, order).astype(bf16)
    member = lax.broadcasted_iota(jnp.int32, (3 * groups, width), 0) % groups
    lane_group = lax.broadcasted_iota(jnp.int32, (3 * groups, width), 1) // states
    shrink_ref[...] = tn(held, jnp.where(member == lane_group, 1.0, 0.0).astype(bf16))

    block = 256 // states
    span, depth = block * states, block * channels
    row_group = lax.broadcasted_iota(jnp.int32, (span, depth), 0) // states
    col_group = lax.broadcasted_iota(jnp.int32, (span, depth), 1) // channels
    mask = row_group == col_group

    def spread(ref, at):
        wide = jnp.concatenate([ref[at : at + span, :]] * block, axis=1)
        return jnp.concatenate(pieces(jnp.where(mask, wide, 0.0), 3), axis=1)

    for n in range(width // span):
        left = moved[:, n * depth : (n + 1) * depth].astype(bf16)
        left = jnp.concatenate([left] * 3, axis=1)
        raw_r = nt(left, spread(in_r_ref, n * span))
        raw_i = nt(left, spread(in_i_ref, n * span))
        at = slice(n * span, (n + 1) * span)
        drive_r, drive_i = complex_times(factor_r[:, at], factor_i[:, at], raw_r, raw_i)
        drive_ref[0, :, at] = drive_r
        drive_ref[1, :, at] = drive_i

    zero = jnp.zeros((lanes_of_chunks, width), f32)

    def body(step, carry):
        state_r, state_i, gone = carry
        rows = pl.ds(pl.multiple_of(step * lanes_of_chunks, lanes_of_chunks), lanes_of_chunks)
        shrink = shrink_ref[rows, :]
        state_r, state_i = advance(
            state_r, state_i, shrink, keep_r, keep_i, drive_ref[0, rows, :], drive_ref[1, rows, :]
        )
        return state_r, state_i, gone * shrink

    state_r, state_i, gone = lax.fori_loop(0, steps, body, (zero, zero, zero + 1.0), unroll=2)
    power_r, power_i = jnp.ones_like(keep_r), jnp.zeros_like(keep_r)
    base_r, base_i, left_over = keep_r, keep_i, steps
    while left_over:
        if left_over & 1:
            power_r, power_i = complex_times(power_r, power_i, base_r, base_i)
        left_over >>= 1
        if left_over:
            base_r, base_i = complex_times(base_r, base_i, base_r, base_i)
    decay_r, decay_i = gone * power_r, gone * power_i
    chunk_ref[0], chunk_ref[1], chunk_ref[2], chunk_ref[3] = decay_r, decay_i, state_r, state_i
    chunk_ref[4] = jnp.broadcast_to(keep_r, zero.shape)
    chunk_ref[5] = jnp.broadcast_to(keep_i, zero.shape)
    all_r, all_i = decay_r[0:1], decay_i[0:1]
    end_r, end_i = state_r[0:1], state_i[0:1]
    for j in range(1, lanes_of_chunks):
        step_r, step_i = decay_r[j : j + 1], decay_i[j : j + 1]
        end_r, end_i = complex_times(step_r, step_i, end_r, end_i)
        end_r, end_i = end_r + state_r[j : j + 1], end_i + state_i[j : j + 1]
        all_r, all_i = complex_times(step_r, step_i, all_r, all_i)
    total_ref[0] = jnp.concatenate([all_r, all_i, end_r, end_i], axis=0)


def read_kernel(
    place_ref, u_ref, drive_ref, shrink_ref, chunk_ref, total_ref, out_r_ref, out_i_ref, skip_ref,
    mixed_ref, state_ref,
):
    tokens, depth = u_ref.shape
    width = shrink_ref.shape[1]
    members = total_ref.shape[0]
    steps = tokens // lanes_of_chunks
    place = place_ref[0]

    def earlier(member, carry):
        carry_r, carry_i = carry
        block = total_ref[member ^ place]
        next_r, next_i = complex_times(block[0:1], block[1:2], carry_r, carry_i)
        return next_r + block[2:3], next_i + block[3:4]

    start = jnp.zeros((1, width), f32)
    carry_r, carry_i = lax.fori_loop(0, place, earlier, (start, start))
    decay_r, decay_i, local_r, local_i = (chunk_ref[k] for k in range(4))
    keep_r, keep_i = chunk_ref[4], chunk_ref[5]
    rows_r, rows_i = [], []
    for j in range(lanes_of_chunks):
        rows_r.append(carry_r)
        rows_i.append(carry_i)
        one = slice(j, j + 1)
        carry_r, carry_i = complex_times(decay_r[one], decay_i[one], carry_r, carry_i)
        carry_r, carry_i = carry_r + local_r[one], carry_i + local_i[one]
    state = (jnp.concatenate(rows_r, axis=0), jnp.concatenate(rows_i, axis=0))

    def body(step, carry):
        rows = pl.ds(pl.multiple_of(step * lanes_of_chunks, lanes_of_chunks), lanes_of_chunks)
        state_r, state_i = advance(
            *carry, shrink_ref[rows, :], keep_r, keep_i, drive_ref[0, rows, :], drive_ref[1, rows, :]
        )
        state_ref[0, rows, :] = state_r
        state_ref[1, rows, :] = state_i
        return state_r, state_i

    lax.fori_loop(0, steps, body, state, unroll=2)
    groups, channels = skip_ref.shape
    states = width // groups
    block = 256 // states
    span, part = block * states, block * channels
    row_group = lax.broadcasted_iota(jnp.int32, (part, span), 0) // channels
    col_group = lax.broadcasted_iota(jnp.int32, (part, span), 1) // states
    mask = row_group == col_group
    outs = []
    for n in range(width // span):
        acc = None
        for k, ref in ((0, out_r_ref), (1, out_i_ref)):
            wide = jnp.concatenate([ref[n * part : (n + 1) * part, :]] * block, axis=1)
            wide = jnp.where(mask, wide, 0.0)
            wide = jnp.concatenate(pieces(-wide if k else wide, 2), axis=0)
            high, low = pieces(state_ref[k, :, n * span : (n + 1) * span], 2)
            first, second = nt(high, wide), nt(low, wide)
            term = first[:, :part] + first[:, part:] + second[:, :part]
            acc = term if acc is None else acc + term
        outs.append(acc)
    total = jnp.concatenate(outs, axis=1)
    order = reorder(tokens)
    total = total + lane_row(skip_ref[...]) * nn(order, u_ref[...])
    mixed = jax.nn.gelu(total).astype(bf16)
    back = tn(order, mixed).astype(bf16)
    rows = mixed_ref.shape[1]
    for k in range(mixed_ref.shape[0]):
        mixed_ref[k] = back[k * rows : (k + 1) * rows]


def whole(shape, dtype=f32):
    return jax.ShapeDtypeStruct(shape, dtype)


def layer_norm(values, scales):
    centered = values - jnp.mean(values, axis=-1, keepdims=True)
    variance = jnp.mean(centered * centered, axis=-1, keepdims=True)
    return centered * lax.rsqrt(variance + 1e-05) * scales


def gather_all(value, axis):
    count = lax.axis_size(axis)
    if not power_of_two(count):
        return None
    distance = 1
    while distance < count:
        value = jnp.concatenate([value, swap(value, axis, distance)], axis=0)
        distance *= 2
    return value


def exchange(blocks, axis, count):
    mine = lax.axis_index(axis)
    if count > 8:
        return lax.all_to_all(blocks, axis, split_axis=0, concat_axis=0, tiled=True)
    came = [lax.dynamic_index_in_dim(blocks, mine, 0, keepdims=True)]
    for distance in range(1, count):
        sent = lax.dynamic_index_in_dim(blocks, (mine + distance) % count, 0, keepdims=True)
        came.append(shift(sent, axis, distance))
    return came


def local(
    mixer_input, retention, decay_real, decay_freq, log_step, input_real, input_imag,
    readout_real, readout_imaginary, skip_weight, norm_gain, projection, residual, mix_gain,
    routes, route_weight, expert_gate, expert_up, expert_down, final_gain,
):
    token_count, depth = mixer_input.shape
    group_count, state_count = decay_real.shape
    channel_count = input_real.shape[2]
    width = group_count * state_count
    tp, sp = lax.axis_size("tp"), lax.axis_size("sp")
    tp_place, sp_place = lax.axis_index("tp"), lax.axis_index("sp")
    row_count = token_count // tp
    mix_width = depth * tp

    proj = projection[None]
    distance = tp // 2
    while distance:
        proj = jnp.concatenate([proj, swap(proj, "tp", distance)], axis=0)
        distance //= 2

    drive, shrink, chunk, total = pl.pallas_call(
        drive_kernel,
        out_shape=(
            whole((2, token_count, width)),
            whole((token_count, width)),
            whole((6, lanes_of_chunks, width)),
            whole((1, 4, width)),
        ),
        cost_estimate=pl.CostEstimate(flops=2 * 10**9, bytes_accessed=4 << 20, transcendentals=0),
        name="drive",
    )(
        mixer_input, retention, decay_real, decay_freq, log_step.reshape(1, group_count),
        input_real.reshape(width, channel_count), input_imag.reshape(width, channel_count),
    )
    totals = gather_all(total, "sp")
    mixed = pl.pallas_call(
        read_kernel,
        out_shape=whole((tp, row_count, depth), bf16),
        in_specs=[pl.BlockSpec(memory_space=pltpu.SMEM)] + [pl.BlockSpec(memory_space=VMEM)] * 8,
        scratch_shapes=[VMEM((2, token_count, width), f32)],
        cost_estimate=pl.CostEstimate(flops=2 * 10**9, bytes_accessed=4 << 20, transcendentals=0),
        name="readout",
    )(
        sp_place.reshape(1), mixer_input, drive, shrink, chunk, totals,
        readout_real.reshape(depth, state_count), readout_imaginary.reshape(depth, state_count),
        skip_weight,
    )

    order = [0]
    distance = tp // 2
    while distance:
        order = order + [k ^ distance for k in order]
        distance //= 2
    came = []
    for k in order:
        sent = lax.dynamic_index_in_dim(mixed, tp_place ^ k, 0, keepdims=False)
        came.append(sent if k == 0 else swap(sent, "tp", k))
    whole_rows = jnp.concatenate(came, axis=1)
    gain = norm_gain.reshape(tp, depth)
    gain = jnp.concatenate([lax.dynamic_index_in_dim(gain, tp_place ^ k, 0) for k in order], axis=1)
    whole_float = whole_rows.astype(f32)
    squares = jnp.sum(whole_float * whole_float, axis=1)
    scaled = (whole_float * gain).astype(bf16)
    summed = jnp.dot(scaled, proj.reshape(mix_width, -1), preferred_element_type=f32)
    mix = summed * lax.rsqrt(squares / mix_width + 1e-06)[:, None]
    hidden = layer_norm(deep_alpha * residual.astype(f32) + mix, mix_gain).astype(bf16)

    capacity = max(2, 2 * row_count * PICKS // sp)
    chosen = routes.reshape(-1)
    onehot = (chosen[:, None] == jnp.arange(sp, dtype=jnp.int32)[None, :]).astype(jnp.int32)
    slot_index = jnp.sum((jnp.cumsum(onehot, axis=0) - 1) * onehot, axis=1)
    target = chosen * capacity + slot_index
    source_row = jnp.full((sp * capacity,), row_count, jnp.int32)
    source_row = source_row.at[target].set(jnp.arange(row_count * PICKS, dtype=jnp.int32) // PICKS)
    padded = jnp.concatenate([hidden, jnp.zeros((1, hidden.shape[1]), hidden.dtype)], axis=0)
    outgoing = padded[source_row].reshape(sp, capacity, -1)
    received = lax.all_to_all(outgoing, "sp", split_axis=0, concat_axis=0, tiled=True)
    arrived = received.reshape(-1, received.shape[2])
    gate_act = jnp.dot(arrived, expert_gate[0], preferred_element_type=f32)
    up_act = jnp.dot(arrived, expert_up[0], preferred_element_type=f32)
    active = (jax.nn.silu(gate_act) * up_act).astype(bf16)
    produced = jnp.dot(active, expert_down[0], preferred_element_type=f32).astype(bf16)
    returned = lax.all_to_all(
        produced.reshape(received.shape), "sp", split_axis=0, concat_axis=0, tiled=True
    )
    gathered_rows = returned.reshape(sp * capacity, -1)[target].reshape(row_count, PICKS, -1)
    expert_mix = jnp.sum(route_weight[:, :, None] * gathered_rows.astype(f32), axis=1)
    layer_out = layer_norm(deep_alpha * hidden.astype(f32) + expert_mix, final_gain)
    return layer_out.astype(bf16)


def solution(mesh):
    in_specs = (
        P("sp", "tp"), P("tp", "sp"), P("tp", None), P("tp", None), P("tp"),
        P("tp", None, None), P("tp", None, None), P("tp", None, None), P("tp", None, None),
        P("tp", None), P(), P("tp", None), P(("sp", "tp"), None), P(),
        P(("sp", "tp"), None), P(("sp", "tp"), None),
        P("sp", None, None), P("sp", None, None), P("sp", None, None), P(),
    )
    out_specs = P(("sp", "tp"), None)
    return jax.shard_map(local, mesh=mesh, in_specs=in_specs, out_specs=out_specs, check_vma=False)
```

```python
import functools

import jax
import jax.numpy as jnp
from jax import lax
from jax.experimental import pallas as pl
from jax.experimental.pallas import tpu as pltpu
from jax.sharding import PartitionSpec as P

PICKS = 2
deep_alpha = 2.0**0.25
lanes_of_chunks = 8
f32, bf16 = jnp.float32, jnp.bfloat16
VMEM = pltpu.VMEM


def power_of_two(count):
    return count & (count - 1) == 0


def swap(value, axis, distance):
    count = lax.axis_size(axis)
    return lax.ppermute(value, axis, [(i, i ^ distance) for i in range(count)])


def shift(value, axis, distance):
    count = lax.axis_size(axis)
    return lax.ppermute(value, axis, [(i, (i + distance) % count) for i in range(count)])


def pieces(value, count):
    out = []
    for _ in range(count):
        piece = value.astype(bf16)
        out.append(piece)
        value = value - piece.astype(f32)
    return out


def nt(left, right):
    return lax.dot_general(left, right, (((1,), (1,)), ((), ())), preferred_element_type=f32)


def nn(left, right):
    return lax.dot_general(left, right, (((1,), (0,)), ((), ())), preferred_element_type=f32)


def tn(left, right):
    return lax.dot_general(left, right, (((0,), (0,)), ((), ())), preferred_element_type=f32)


def reorder(count):
    steps = count // lanes_of_chunks
    row = lax.broadcasted_iota(jnp.int32, (count, count), 0)
    col = lax.broadcasted_iota(jnp.int32, (count, count), 1)
    source = (row % lanes_of_chunks) * steps + row // lanes_of_chunks
    return jnp.where(col == source, 1.0, 0.0).astype(bf16)


def lane_row(value):
    groups, width = value.shape
    per = 128 // width
    wide = jnp.concatenate([value] * per, axis=1)
    spot = lax.broadcasted_iota(jnp.int32, (1, 128), 1) // width
    parts = []
    for q in range(groups // per):
        row = wide[q * per : q * per + 1]
        for m in range(1, per):
            row = jnp.where(spot == m, wide[q * per + m : q * per + m + 1], row)
        parts.append(row)
    return jnp.concatenate(parts, axis=1)


def complex_times(ar, ai, br, bi):
    return ar * br - ai * bi, ar * bi + ai * br


def less_one(value):
    near = jnp.ones_like(value)
    for k in range(11, 1, -1):
        near = 1.0 + near * value / k
    return jnp.where(jnp.abs(value) < 0.5, near * value, jnp.exp(value) - 1.0)


def advance(block_r, block_i, shrink, keep_r, keep_i, drive_r, drive_i):
    turned_r, turned_i = complex_times(keep_r, keep_i, block_r, block_i)
    return shrink * turned_r + drive_r, shrink * turned_i + drive_i


def drive_kernel(
    u_ref, held_ref, real_ref, freq_ref, step_ref, in_r_ref, in_i_ref,
    drive_ref, shrink_ref, chunk_ref, total_ref,
):
    tokens, _ = u_ref.shape
    groups, states = real_ref.shape
    channels = in_r_ref.shape[0] // groups
    width = groups * states
    steps = tokens // lanes_of_chunks
    log_step = step_ref[...]
    eye = lax.broadcasted_iota(jnp.int32, (groups, groups), 0) == lax.broadcasted_iota(
        jnp.int32, (groups, groups), 1
    )
    log_column = jnp.sum(jnp.where(eye, log_step, 0.0), axis=1, keepdims=True)
    stride = jnp.exp(log_column)
    decay_real, decay_freq = real_ref[...], freq_ref[...]
    growth = decay_real * stride
    turning = decay_freq * stride
    size = jnp.exp(growth)
    cosine, sine, half = jnp.cos(turning), jnp.sin(turning), jnp.sin(0.5 * turning)
    upper_real = less_one(growth) * cosine - 2.0 * half * half
    upper_imag = size * sine
    denominator = decay_real * decay_real + decay_freq * decay_freq
    factor_real = (upper_real * decay_real + upper_imag * decay_freq) / denominator
    factor_imag = (upper_imag * decay_real - upper_real * decay_freq) / denominator
    keep_r, keep_i = lane_row(size * cosine), lane_row(upper_imag)
    factor_r, factor_i = lane_row(factor_real), lane_row(factor_imag)

    order = reorder(tokens)
    moved = nn(order, u_ref[...])
    held = jnp.concatenate(pieces(jnp.exp(held_ref[...]), 3), axis=0)
    held = nt(held, order).astype(bf16)
    member = lax.broadcasted_iota(jnp.int32, (3 * groups, width), 0) % groups
    lane_group = lax.broadcasted_iota(jnp.int32, (3 * groups, width), 1) // states
    shrink_ref[...] = tn(held, jnp.where(member == lane_group, 1.0, 0.0).astype(bf16))

    block = 256 // states
    span, depth = block * states, block * channels
    row_group = lax.broadcasted_iota(jnp.int32, (depth, span), 0) // channels
    col_group = lax.broadcasted_iota(jnp.int32, (depth, span), 1) // states
    mask = row_group == col_group

    def spread(ref, at):
        wide = jnp.concatenate([ref[at : at + depth, :]] * block, axis=1)
        return jnp.concatenate(pieces(jnp.where(mask, wide, 0.0), 3), axis=0)

    for n in range(width // span):
        left = moved[:, n * depth : (n + 1) * depth].astype(bf16)
        left = jnp.concatenate([left] * 3, axis=1)
        raw_r = nn(left, spread(in_r_ref, n * depth))
        raw_i = nn(left, spread(in_i_ref, n * depth))
        at = slice(n * span, (n + 1) * span)
        drive_r, drive_i = complex_times(factor_r[:, at], factor_i[:, at], raw_r, raw_i)
        drive_ref[0, :, at] = drive_r
        drive_ref[1, :, at] = drive_i

    zero = jnp.zeros((lanes_of_chunks, width), f32)

    def body(step, carry):
        state_r, state_i, gone = carry
        rows = pl.ds(pl.multiple_of(step * lanes_of_chunks, lanes_of_chunks), lanes_of_chunks)
        shrink = shrink_ref[rows, :]
        state_r, state_i = advance(
            state_r, state_i, shrink, keep_r, keep_i, drive_ref[0, rows, :], drive_ref[1, rows, :]
        )
        return state_r, state_i, gone * shrink

    state_r, state_i, gone = lax.fori_loop(0, steps, body, (zero, zero, zero + 1.0), unroll=2)
    power_r, power_i = jnp.ones_like(keep_r), jnp.zeros_like(keep_r)
    base_r, base_i, left_over = keep_r, keep_i, steps
    while left_over:
        if left_over & 1:
            power_r, power_i = complex_times(power_r, power_i, base_r, base_i)
        left_over >>= 1
        if left_over:
            base_r, base_i = complex_times(base_r, base_i, base_r, base_i)
    decay_r, decay_i = gone * power_r, gone * power_i
    chunk_ref[0], chunk_ref[1], chunk_ref[2], chunk_ref[3] = decay_r, decay_i, state_r, state_i
    chunk_ref[4] = jnp.broadcast_to(keep_r, zero.shape)
    chunk_ref[5] = jnp.broadcast_to(keep_i, zero.shape)
    all_r, all_i = decay_r[0:1], decay_i[0:1]
    end_r, end_i = state_r[0:1], state_i[0:1]
    for j in range(1, lanes_of_chunks):
        step_r, step_i = decay_r[j : j + 1], decay_i[j : j + 1]
        end_r, end_i = complex_times(step_r, step_i, end_r, end_i)
        end_r, end_i = end_r + state_r[j : j + 1], end_i + state_i[j : j + 1]
        all_r, all_i = complex_times(step_r, step_i, all_r, all_i)
    total_ref[0] = jnp.concatenate([all_r, all_i, end_r, end_i], axis=0)


def read_kernel(
    place_ref, u_ref, drive_ref, shrink_ref, chunk_ref, near_ref, far_ref, out_r_ref, out_i_ref,
    skip_ref, *rest,
):
    *mixed_refs, state_ref, total_ref, back_ref = rest
    tokens, depth = u_ref.shape
    width = shrink_ref.shape[1]
    half = near_ref.shape[0]
    total_ref[:half] = near_ref[...]
    total_ref[half:] = far_ref[...]
    steps = tokens // lanes_of_chunks
    place = place_ref[0]

    def earlier(member, carry):
        carry_r, carry_i = carry
        block = total_ref[member ^ place]
        next_r, next_i = complex_times(block[0:1], block[1:2], carry_r, carry_i)
        return next_r + block[2:3], next_i + block[3:4]

    start = jnp.zeros((1, width), f32)
    carry_r, carry_i = lax.fori_loop(0, place, earlier, (start, start))
    decay_r, decay_i, local_r, local_i = (chunk_ref[k] for k in range(4))
    keep_r, keep_i = chunk_ref[4], chunk_ref[5]
    rows_r, rows_i = [], []
    for j in range(lanes_of_chunks):
        rows_r.append(carry_r)
        rows_i.append(carry_i)
        one = slice(j, j + 1)
        carry_r, carry_i = complex_times(decay_r[one], decay_i[one], carry_r, carry_i)
        carry_r, carry_i = carry_r + local_r[one], carry_i + local_i[one]
    state = (jnp.concatenate(rows_r, axis=0), jnp.concatenate(rows_i, axis=0))

    def body(step, carry):
        rows = pl.ds(pl.multiple_of(step * lanes_of_chunks, lanes_of_chunks), lanes_of_chunks)
        state_r, state_i = advance(
            *carry, shrink_ref[rows, :], keep_r, keep_i, drive_ref[0, rows, :], drive_ref[1, rows, :]
        )
        state_ref[0, rows, :] = state_r
        state_ref[1, rows, :] = state_i
        return state_r, state_i

    lax.fori_loop(0, steps, body, state, unroll=2)
    groups, channels = skip_ref.shape
    states = width // groups
    block = 256 // states
    span, part = block * states, block * channels
    row_group = lax.broadcasted_iota(jnp.int32, (part, span), 0) // channels
    col_group = lax.broadcasted_iota(jnp.int32, (part, span), 1) // states
    mask = row_group == col_group
    outs = []
    for n in range(width // span):
        acc = None
        for k, ref in ((0, out_r_ref), (1, out_i_ref)):
            wide = jnp.concatenate([ref[n * part : (n + 1) * part, :]] * block, axis=1)
            wide = jnp.where(mask, wide, 0.0)
            wide = jnp.concatenate(pieces(-wide if k else wide, 2), axis=0)
            high, low = pieces(state_ref[k, :, n * span : (n + 1) * span], 2)
            first, second = nt(high, wide), nt(low, wide)
            term = first[:, :part] + first[:, part:] + second[:, :part]
            acc = term if acc is None else acc + term
        outs.append(acc)
    total = jnp.concatenate(outs, axis=1)
    order = reorder(tokens)
    total = total + lane_row(skip_ref[...]) * nn(order, u_ref[...])
    mixed = jax.nn.gelu(total).astype(bf16)
    back_ref[...] = tn(order, mixed).astype(bf16)
    rows = mixed_refs[0].shape[0]
    for ref, k in zip(mixed_refs, doubling(len(mixed_refs))):
        at = pl.multiple_of((place_ref[1] ^ k) * rows, rows)
        ref[...] = back_ref[pl.ds(at, rows), :]


def doubling(count):
    order, distance = [0], count // 2
    while distance:
        order = order + [k ^ distance for k in order]
        distance //= 2
    return order


def whole(shape, dtype=f32):
    return jax.ShapeDtypeStruct(shape, dtype)


def layer_norm(values, scales):
    centered = values - jnp.mean(values, axis=-1, keepdims=True)
    variance = jnp.mean(centered * centered, axis=-1, keepdims=True)
    return centered * lax.rsqrt(variance + 1e-05) * scales


def route_kernel(capacity, relative, place_ref, routes_ref, weight_ref, pick_ref, join_ref):
    rows, picks = routes_ref.shape
    slots = pick_ref.shape[0]
    experts = slots // capacity
    routes = routes_ref[...]
    if relative:
        routes = routes ^ place_ref[0]
    iota = functools.partial(lax.broadcasted_iota, jnp.int32)
    eye = jnp.where(iota((rows, rows), 0) == iota((rows, rows), 1), 1.0, 0.0).astype(bf16)
    before = jnp.where(iota((rows, rows), 0) < iota((rows, rows), 1), 1.0, 0.0).astype(bf16)
    chosen = tn(routes.astype(f32).astype(bf16), eye)
    weight = sum(tn(piece, eye) for piece in pieces(weight_ref[...], 3))
    expert = iota((experts, rows), 0).astype(f32)
    named, share = 0.0, 0.0
    for k in range(picks):
        hit = expert == chosen[k : k + 1]
        named = named + jnp.where(hit, 1.0, 0.0)
        share = share + jnp.where(hit, weight[k : k + 1], 0.0)
    slot = nn(named.astype(bf16), before)
    owner = jnp.where(iota((slots, experts), 0) // capacity == iota((slots, experts), 1), 1.0, 0.0)
    owner = owner.astype(bf16)
    place = (iota((slots, rows), 0) % capacity).astype(f32)
    picked = (nn(owner, slot.astype(bf16)) == place) & (nn(owner, named.astype(bf16)) > 0.5)
    pick_ref[...] = jnp.where(picked, 1.0, 0.0).astype(bf16)
    shares = sum(nn(owner, piece) for piece in pieces(share, 3))
    join_ref[...] = jnp.concatenate(pieces(jnp.where(picked, shares, 0.0), 3), axis=1)


def hidden_kernel(
    count, place_ref, gain_ref, residual_ref, mix_gain_ref, pick_ref, *rest
):
    parts, projs, rest = rest[:count], rest[count : 2 * count], rest[2 * count :]
    hidden_ref, *out_refs, proj_ref, sems = rest
    depth = parts[0].shape[1]
    copies = []
    for k in range(count):
        copy = pltpu.make_async_copy(projs[k], proj_ref.at[k], sems.at[k])
        copy.start()
        copies.append(copy)
    squares, total = 0.0, 0.0
    for k, distance in enumerate(doubling(count)):
        part = parts[k][...].astype(f32)
        squares = squares + jnp.sum(part * part, axis=1, keepdims=True)
        scaled = (part * gain_ref[pl.ds(place_ref[1] ^ distance, 1), :]).astype(bf16)
        copies[k].wait()
        total = total + nn(scaled, proj_ref[k])
    mix = total * lax.rsqrt(squares / (depth * count) + 1e-06)
    hidden = layer_norm(deep_alpha * residual_ref[...].astype(f32) + mix, mix_gain_ref[...])
    hidden = hidden.astype(bf16)
    hidden_ref[...] = hidden
    start = 0
    for ref in out_refs:
        size = ref.shape[0]
        ref[...] = nn(pick_ref[start : start + size, :], hidden).astype(bf16)
        start += size


def expert_kernel(count, gate_ref, up_ref, down_ref, *rest):
    in_refs, out_refs, (rows_ref, sum_ref) = rest[:count], rest[count : 2 * count], rest[2 * count :]
    size = in_refs[0].shape[0]
    step = pl.program_id(0)

    @pl.when(step == 0)
    def _():
        for k, ref in enumerate(in_refs):
            rows_ref[k * size : (k + 1) * size, :] = ref[...]
        sum_ref[...] = jnp.zeros_like(sum_ref)

    rows = rows_ref[...]
    active = (jax.nn.silu(nn(rows, gate_ref[0])) * nn(rows, up_ref[0])).astype(bf16)
    sum_ref[...] += nn(active, down_ref[0])

    @pl.when(step == pl.num_programs(0) - 1)
    def _():
        for k, ref in enumerate(out_refs):
            ref[...] = sum_ref[k * size : (k + 1) * size, :].astype(bf16)


def experts(blocks, gate, up, down):
    _, width, inner = gate.shape
    size = blocks[0].shape[0]
    count = len(blocks)
    tile = min(inner, 256)
    full = pl.BlockSpec((size, width), lambda h: (0, 0))
    return pl.pallas_call(
        functools.partial(expert_kernel, count),
        grid=(inner // tile,),
        out_shape=[whole((size, width), bf16)] * count,
        in_specs=[
            pl.BlockSpec((1, width, tile), lambda h: (0, 0, h)),
            pl.BlockSpec((1, width, tile), lambda h: (0, 0, h)),
            pl.BlockSpec((1, tile, width), lambda h: (0, h, 0)),
        ]
        + [full] * count,
        out_specs=[full] * count,
        scratch_shapes=[VMEM((count * size, width), bf16), VMEM((count * size, width), f32)],
        cost_estimate=pl.CostEstimate(flops=10**9, bytes_accessed=6 << 20, transcendentals=0),
        name="experts",
    )(gate, up, down, *blocks)


def final_kernel(hidden_ref, join_ref, gain_ref, *rest):
    *in_refs, out_ref, rows_ref = rest
    rows = hidden_ref.shape[0]
    start = 0
    for ref in in_refs:
        rows_ref[start : start + ref.shape[0], :] = ref[...]
        start += ref.shape[0]
    parts = tn(join_ref[...], rows_ref[...])
    expert_mix = parts[:rows] + parts[rows : 2 * rows] + parts[2 * rows :]
    values = deep_alpha * hidden_ref[...].astype(f32) + expert_mix
    out_ref[...] = layer_norm(values, gain_ref[...]).astype(bf16)


def local(
    mixer_input, retention, decay_real, decay_freq, log_step, input_real, input_imag,
    readout_real, readout_imaginary, skip_weight, norm_gain, projection, residual, mix_gain,
    routes, route_weight, expert_gate, expert_up, expert_down, final_gain,
):
    token_count, depth = mixer_input.shape
    group_count, state_count = decay_real.shape
    width = group_count * state_count
    tp, sp = lax.axis_size("tp"), lax.axis_size("sp")
    place = jnp.stack([lax.axis_index("sp"), lax.axis_index("tp")])
    row_count, model = residual.shape
    smem, vmem = pl.BlockSpec(memory_space=pltpu.SMEM), pl.BlockSpec(memory_space=VMEM)
    hbm = pl.BlockSpec(memory_space=pl.ANY)
    cost = functools.partial(pl.CostEstimate, transcendentals=0)

    proj = {0: projection}
    distance = tp // 2
    proj[distance] = swap(projection, "tp", distance)

    drive, shrink, chunk, total = pl.pallas_call(
        drive_kernel,
        out_shape=(
            whole((2, token_count, width)),
            whole((token_count, width)),
            whole((6, lanes_of_chunks, width)),
            whole((1, 4, width)),
        ),
        cost_estimate=cost(flops=2 * 10**9, bytes_accessed=4 << 20),
        name="drive",
    )(
        mixer_input, retention, decay_real, decay_freq, log_step.reshape(1, group_count),
        input_real.transpose(0, 2, 1).reshape(depth, state_count),
        input_imag.transpose(0, 2, 1).reshape(depth, state_count),
    )

    near, far, distance = total, None, 1
    while distance < sp:
        if far is not None:
            near = jnp.concatenate([near, far], axis=0)
        far = swap(near, "sp", distance)
        distance *= 2

    capacity = max(2, 2 * row_count * PICKS // sp)
    relative = sp <= 8
    late_routes, _ = lax.optimization_barrier((routes, total))
    pick, join = pl.pallas_call(
        functools.partial(route_kernel, capacity, relative),
        out_shape=(
            whole((sp * capacity, row_count), bf16),
            whole((sp * capacity, 3 * row_count), bf16),
        ),
        in_specs=[smem, vmem, vmem],
        cost_estimate=cost(flops=10**8, bytes_accessed=1 << 17),
        name="route",
    )(place, late_routes, route_weight)

    mixed = pl.pallas_call(
        read_kernel,
        out_shape=[whole((row_count, depth), bf16)] * tp,
        in_specs=[smem] + [vmem] * 9,
        scratch_shapes=[
            VMEM((2, token_count, width), f32),
            VMEM((sp, 4, width), f32),
            VMEM((token_count, depth), bf16),
        ],
        cost_estimate=cost(flops=2 * 10**9, bytes_accessed=4 << 20),
        name="readout",
    )(
        place, mixer_input, drive, shrink, chunk, near, far,
        readout_real.reshape(depth, state_count), readout_imaginary.reshape(depth, state_count),
        skip_weight,
    )

    parts = [part if k == 0 else swap(part, "tp", k) for part, k in zip(mixed, doubling(tp))]
    distance = tp // 2
    held = [projection, lax.optimization_barrier((proj[distance], mixed[0]))[0]]
    held[0] = lax.optimization_barrier((projection, mixed[0]))[0]
    proj[distance] = held[1]
    sources = dict(proj)
    sources[0] = held[0]
    distance //= 2
    while distance:
        for k in list(sources):
            sources[k ^ distance] = swap(sources[k], "tp", distance)
        distance //= 2
    sources[0] = projection

    blocks = sp if relative else 1
    hidden, *outgoing = pl.pallas_call(
        functools.partial(hidden_kernel, tp),
        out_shape=[whole((row_count, model), bf16)]
        + [whole((sp * capacity // blocks, model), bf16)] * blocks,
        in_specs=[smem] + [vmem] * (4 + tp) + [hbm] * tp,
        scratch_shapes=[VMEM((tp, depth, model), bf16), pltpu.SemaphoreType.DMA((tp,))],
        cost_estimate=cost(flops=10**9, bytes_accessed=6 << 20),
        name="hidden",
    )(
        place, norm_gain.reshape(tp, depth), residual, mix_gain.reshape(1, model), pick,
        *parts, *[sources[k] for k in doubling(tp)],
    )

    weights = (expert_gate, expert_up, expert_down)
    if relative:
        half = sp // 2
        order = list(range(half, sp)) + list(range(1, half))
        came = {k: swap(outgoing[k], "sp", k) for k in order}
        came[0] = outgoing[0]
        back = {}
        sets = [list(range(half)), list(range(half, half + half // 2)), list(range(half + half // 2, sp))]
        for members in sets:
            made = experts([came[k] for k in members], *weights)
            for k, block in zip(members, made):
                back[k] = swap(block, "sp", k) if k else block
        returned = [back[k] for k in range(sp)]
    else:
        trade = functools.partial(
            lax.all_to_all, axis_name="sp", split_axis=0, concat_axis=0, tiled=True
        )
        came = trade(outgoing[0].reshape(sp, capacity, model)).reshape(-1, model)
        made = experts([came], *weights)[0]
        returned = [trade(made.reshape(sp, capacity, model)).reshape(-1, model)]
    return pl.pallas_call(
        final_kernel,
        out_shape=whole((row_count, model), bf16),
        scratch_shapes=[VMEM((sp * capacity, model), bf16)],
        cost_estimate=cost(flops=10**9, bytes_accessed=2 << 20),
        name="final",
    )(hidden, join, final_gain.reshape(1, model), *returned)


def solution(mesh):
    in_specs = (
        P("sp", "tp"), P("tp", "sp"), P("tp", None), P("tp", None), P("tp"),
        P("tp", None, None), P("tp", None, None), P("tp", None, None), P("tp", None, None),
        P("tp", None), P(), P("tp", None), P(("sp", "tp"), None), P(),
        P(("sp", "tp"), None), P(("sp", "tp"), None),
        P("sp", None, None), P("sp", None, None), P("sp", None, None), P(),
    )
    out_specs = P(("sp", "tp"), None)
    return jax.shard_map(local, mesh=mesh, in_specs=in_specs, out_specs=out_specs, check_vma=False)
```
